32 devices in a mesh: gr: 2 (over x), sp: 8 (over z, y), tp: 2 (over core).
Axes of the slice: x: 2, y: 2, z: 4, core: 2. Of those that a mesh axis runs over, the one named last changes fastest.
Arguments:
- tokens: bfloat16 [8, 1536, 2048], P('gr', 'sp'), parts along dimension 0, may hold values from -6 to 6
- key_weight: bfloat16 [2048, 512], P(None, 'tp'), may hold values from -0.125 to 0.125
- value_weight: bfloat16 [2048, 1024], P(None, 'tp'), may hold values from -0.125 to 0.125
- input_weight: bfloat16 [2048, 8], P(None, 'tp'), may hold values from -0.125 to 0.125
- forget_weight: bfloat16 [2048, 8], P(None, 'tp'), may hold values from -0.125 to 0.125
- forget_bias: float32 [8], P('tp'), may hold values from 2.5 to 9.5
- query: bfloat16 [8, 512], P('gr', 'tp'), parts along dimension 0, may hold values from -6 to 6
Outputs:
- key_cache: bfloat16 [16, 768, 512], P(('gr', 'sp'), None, 'tp'), parts along dimension 0
- value_cache: bfloat16 [16, 768, 1024], P(('gr', 'sp'), None, 'tp'), parts along dimension 0
- memory: float32 [8, 8, 64, 128], P('gr', 'tp'), parts along dimension 0
- normalizer: float32 [8, 8, 64], P('gr', 'tp'), parts along dimension 0
- stabilizer: float32 [8, 8], P('gr', 'tp'), parts along dimension 0
- first_read: float32 [8, 1024], P('gr', 'tp'), parts along dimension 0
The draws below stay inside these ranges and needn't reach their ends.
There are 2 independent parts, one for each index of `gr`. The reference program is written for one: setup_inputs(seed, part) draws one part's arguments, and reference() takes and returns one part's arrays. A program takes and returns all parts, laid end to end along the dimension named above; an argument that names none is the same for every part. Nothing has to cross between parts.
All inputs are finite; a program needn't handle non-finite values.
Results may differ from the reference program's by a relative error of at most 0.0015.
The reference program's roundings to bfloat16 on the way (of `keys` and `values`) count: a program that leaves them out, or rounds other values in their place, can miss the bound.
Values may be sent and summed in bfloat16 or wider, within the bound.
A program may use at most 64 MiB of HBM per device.

```python
import jax
import jax.numpy as jnp
from jax import lax

D = 2048
H = 8
DK = 64
DV = 128
SEQS = 4
LEN = 1536
N_SP = 8


def draw_forget_bias(key, part):
    pick, lower, upper = jax.random.split(jax.random.fold_in(key, 17), 3)
    share = 0.5
    slow = jax.random.uniform(pick, (H,), jnp.float32) < share
    fast_value = jax.random.uniform(lower, (H,), jnp.float32, 2.5, 3.5)
    slow_value = jax.random.uniform(upper, (H,), jnp.float32, 8.5, 9.5)
    return jnp.where(slow, slow_value, fast_value).astype(jnp.float32)


def levels(rng, extent, cuts, least, high):
    def one(axis_at, parts):
        heights = jax.random.uniform(jax.random.fold_in(jax.random.fold_in(rng, 6), axis_at), (parts,), jnp.float32, least / len(cuts), high / len(cuts))
        return jnp.repeat(jnp.exp(heights), extent[axis_at] // parts).reshape((-1,) + (1,) * (len(extent) - axis_at - 1))

    level = one(*cuts[0])
    for cut in cuts[1:]:
        level = level * one(*cut)
    return level


def normal_values(key, extent, scale, bound, cuts=(), dtype=jnp.bfloat16):
    loudness = levels(key, extent, cuts, -0.22, 0.18) if cuts else 1.0
    drawn = jax.random.normal(key, extent, jnp.float32) * scale * loudness
    return jnp.minimum(jnp.maximum(drawn, -bound), bound).astype(dtype)


def setup_inputs(seed: int = 0, part: int = 0) -> dict:
    key_of = jax.random.split(jax.random.key(seed), 8)
    part_splits = jax.random.split(jax.random.fold_in(key_of[7], part), 8)
    tokens = normal_values(part_splits[0], (SEQS, LEN, D), 1.0, 6.0, ((1, 8),))
    key_weight = normal_values(key_of[1], (D, H * DK), D ** -0.5, 0.125, ((1, 2),))
    value_weight = normal_values(key_of[2], (D, H * DV), D ** -0.5, 0.125, ((1, 2),))
    input_weight = normal_values(key_of[3], (D, H), D ** -0.5, 0.125, ((1, 2),))
    forget_weight = normal_values(key_of[4], (D, H), D ** -0.5, 0.125, ((1, 2),))
    forget_bias = draw_forget_bias(jax.random.fold_in(key_of[7], 71), part)
    query = normal_values(part_splits[6], (SEQS, H * DK), 1.0, 6.0, ((1, 2),))
    return dict(tokens=tokens, key_weight=key_weight, value_weight=value_weight, input_weight=input_weight, forget_weight=forget_weight, forget_bias=forget_bias, query=query)


def reference(tokens, key_weight, value_weight, input_weight, forget_weight, forget_bias, query):
    seqs, length, width = tokens.shape
    heads = input_weight.shape[1]
    kdim = key_weight.shape[1] // heads
    vdim = value_weight.shape[1] // heads
    pieces = N_SP // seqs
    sub = length // N_SP // pieces
    flat = tokens.reshape(seqs * length, width)
    keys = jnp.dot(flat, key_weight, preferred_element_type=jnp.float32).astype(jnp.bfloat16)
    values = jnp.dot(flat, value_weight, preferred_element_type=jnp.float32).astype(jnp.bfloat16)
    igate = jnp.dot(flat, input_weight, preferred_element_type=jnp.float32).reshape(seqs, length, heads)
    fpre = jnp.dot(flat, forget_weight, preferred_element_type=jnp.float32) + forget_bias.astype(jnp.float32)
    logf = jax.nn.log_sigmoid(fpre).reshape(seqs, length, heads)
    total = jnp.sum(logf, axis=1)
    logw = total[:, None, :] - jnp.cumsum(logf, axis=1) + igate
    stabilizer = jnp.maximum(total, jnp.max(logw, axis=1))
    weight = jnp.exp(logw - stabilizer[:, None, :]) * (kdim ** -0.5)
    keys4 = keys.reshape(seqs, length, heads, kdim).astype(jnp.float32)
    values4 = values.reshape(seqs, length, heads, vdim).astype(jnp.float32)
    scaled = keys4 * weight[..., None]
    memory = jnp.einsum('slhd,slhe->shde', scaled, values4, precision=lax.Precision.HIGHEST)
    normalizer = jnp.sum(scaled, axis=1)
    asked = query.astype(jnp.float32).reshape(seqs, heads, kdim)
    numer = jnp.einsum('shd,shde->she', asked, memory, precision=lax.Precision.HIGHEST)
    denom = jnp.maximum(jnp.abs(jnp.sum(asked * normalizer, axis=-1)), 1.0)
    first_read = (numer / denom[..., None]).reshape(seqs, heads * vdim)

    def arrange(rows):
        cols = rows.shape[-1]
        grid = rows.reshape(seqs, N_SP, pieces, sub, cols)
        return jnp.transpose(grid, (0, 2, 1, 3, 4)).reshape(seqs * pieces, N_SP * sub, cols)

    return (arrange(keys.reshape(seqs, length, heads * kdim)), arrange(values.reshape(seqs, length, heads * vdim)),
            memory, normalizer, stabilizer, first_read)
```

```python
import jax
import jax.numpy as jnp
from jax import lax
from jax.sharding import PartitionSpec as P

HIGH = lax.Precision.HIGHEST


def local(tokens, key_weight, value_weight, input_weight, forget_weight, forget_bias, query):
    seqs, span, width = tokens.shape
    heads = input_weight.shape[1]
    kdim = key_weight.shape[1] // heads
    vdim = value_weight.shape[1] // heads
    size = lax.axis_size("sp")
    me = lax.axis_index("sp")
    pieces = size // seqs
    sub = span // pieces
    rows = heads * kdim // pieces
    flat = tokens.reshape(seqs * span, width)
    gate_pair = jnp.concatenate([input_weight, forget_weight], axis=1)
    gates = lax.dot_general(gate_pair, flat, (((0,), (1,)), ((), ())), preferred_element_type=jnp.float32)
    igate = gates[:heads]
    logf = jax.nn.log_sigmoid(gates[heads:] + forget_bias[:, None])
    packet = jnp.concatenate([igate, logf]).reshape(2 * heads, seqs, span).transpose(1, 0, 2)
    packet = jnp.repeat(packet, pieces, axis=0)
    packet = lax.all_to_all(packet, "sp", split_axis=0, concat_axis=0, tiled=True)
    values = jnp.dot(flat, value_weight, preferred_element_type=jnp.float32).astype(jnp.bfloat16)
    keys = jnp.dot(flat, key_weight, preferred_element_type=jnp.float32).astype(jnp.bfloat16)
    value_cache = lax.all_to_all(
        values.reshape(size, sub, heads * vdim), "sp", split_axis=0, concat_axis=1, tiled=True
    )
    key_cache = lax.all_to_all(
        keys.reshape(size, sub, heads * kdim), "sp", split_axis=0, concat_axis=1, tiled=True
    )
    igate, logf = packet[:, :heads], packet[:, heads:]
    at = jnp.arange(span)
    behind = (at[:, None] > at[None, :]).astype(jnp.float32)
    after = jnp.einsum("pht,ts->phs", logf, behind, precision=HIGH)
    sums = jnp.sum(logf, axis=2)
    block = jnp.arange(size)
    later = jnp.sum(jnp.where(block[:, None, None] > block[None, :, None], sums[:, None, :], 0.0), axis=0)
    total = jnp.sum(sums, axis=0)
    logw = after + later[:, :, None] + igate
    stabilizer = jnp.maximum(total, jnp.max(logw, axis=(0, 2)))
    mine = lax.dynamic_slice_in_dim(logw, lax.rem(me, pieces) * sub, sub, axis=2)
    weight = jnp.exp(mine - stabilizer[None, :, None]) * kdim ** (-0.5)
    weight = weight.transpose(0, 2, 1).reshape(size * sub, heads, 1)
    scaled = key_cache.reshape(size * sub, heads, kdim).astype(jnp.float32) * weight
    kept = value_cache.reshape(size * sub, heads, vdim).astype(jnp.float32)
    memory = jnp.einsum("lhd,lhe->hde", scaled, kept, precision=HIGH)
    normal = jnp.sum(scaled, axis=0).reshape(pieces, 1, rows)
    fill = jnp.zeros((pieces, 6, vdim), jnp.float32)
    tail = jnp.pad(normal, ((0, 0), (0, 0), (0, vdim - rows)))
    level = jnp.broadcast_to(jnp.pad(stabilizer, (0, vdim - heads)) / pieces, (pieces, 1, vdim))
    share = jnp.concatenate([memory.reshape(pieces, rows, vdim), tail, level, fill], axis=1)
    groups = [[s * pieces + b for b in range(pieces)] for s in range(seqs)]
    share = lax.all_to_all(share, "sp", split_axis=0, concat_axis=0, tiled=True, axis_index_groups=groups)
    share = jnp.sum(share, axis=0)
    every = lax.all_gather(share, "sp").reshape(seqs, pieces, rows + 8, vdim)
    memory = every[:, :, :rows].reshape(seqs, heads, kdim, vdim)
    normalizer = every[:, :, rows, :rows].reshape(seqs, heads, kdim)
    stabilizer = every[:, 0, rows + 1, :heads]
    asked = query.astype(jnp.float32).reshape(seqs, heads, kdim)
    numer = jnp.sum(asked[..., None] * memory, axis=2)
    denom = jnp.maximum(jnp.abs(jnp.sum(asked * normalizer, axis=-1)), 1.0)
    first_read = (numer / denom[..., None]).reshape(seqs, heads * vdim)
    return (key_cache, value_cache, memory, normalizer, stabilizer, first_read)


def solution(mesh):
    return jax.shard_map(
        local,
        mesh=mesh,
        in_specs=(
            P("gr", "sp", None),
            P(None, "tp"),
            P(None, "tp"),
            P(None, "tp"),
            P(None, "tp"),
            P("tp"),
            P("gr", "tp"),
        ),
        out_specs=(
            P(("gr", "sp"), None, "tp"),
            P(("gr", "sp"), None, "tp"),
            P("gr", "tp", None, None),
            P("gr", "tp", None),
            P("gr", "tp"),
            P("gr", "tp"),
        ),
        check_vma=False,
    )
```

```python
import functools

import jax
import jax.numpy as jnp
from jax import lax
from jax.experimental import pallas as pl
from jax.experimental.pallas import tpu as pltpu
from jax.sharding import PartitionSpec as P

HIGH = lax.Precision.HIGHEST


def plain(tokens, key_weight, value_weight, input_weight, forget_weight, forget_bias, query):
    seqs, span, width = tokens.shape
    heads = input_weight.shape[1]
    kdim = key_weight.shape[1] // heads
    vdim = value_weight.shape[1] // heads
    size = lax.axis_size("sp")
    me = lax.axis_index("sp")
    pieces = size // seqs
    sub = span // pieces
    rows = heads * kdim // pieces
    flat = tokens.reshape(seqs * span, width)
    gate_pair = jnp.concatenate([input_weight, forget_weight], axis=1)
    gates = lax.dot_general(gate_pair, flat, (((0,), (1,)), ((), ())), preferred_element_type=jnp.float32)
    igate = gates[:heads]
    logf = jax.nn.log_sigmoid(gates[heads:] + forget_bias[:, None])
    packet = jnp.concatenate([igate, logf]).reshape(2 * heads, seqs, span).transpose(1, 0, 2)
    packet = jnp.repeat(packet, pieces, axis=0)
    packet = lax.all_to_all(packet, "sp", split_axis=0, concat_axis=0, tiled=True)
    values = jnp.dot(flat, value_weight, preferred_element_type=jnp.float32).astype(jnp.bfloat16)
    keys = jnp.dot(flat, key_weight, preferred_element_type=jnp.float32).astype(jnp.bfloat16)
    value_cache = lax.all_to_all(
        values.reshape(size, sub, heads * vdim), "sp", split_axis=0, concat_axis=1, tiled=True
    )
    key_cache = lax.all_to_all(
        keys.reshape(size, sub, heads * kdim), "sp", split_axis=0, concat_axis=1, tiled=True
    )
    igate, logf = packet[:, :heads], packet[:, heads:]
    at = jnp.arange(span)
    behind = (at[:, None] > at[None, :]).astype(jnp.float32)
    after = jnp.einsum("pht,ts->phs", logf, behind, precision=HIGH)
    sums = jnp.sum(logf, axis=2)
    block = jnp.arange(size)
    later = jnp.sum(jnp.where(block[:, None, None] > block[None, :, None], sums[:, None, :], 0.0), axis=0)
    total = jnp.sum(sums, axis=0)
    logw = after + later[:, :, None] + igate
    stabilizer = jnp.maximum(total, jnp.max(logw, axis=(0, 2)))
    mine = lax.dynamic_slice_in_dim(logw, lax.rem(me, pieces) * sub, sub, axis=2)
    weight = jnp.exp(mine - stabilizer[None, :, None]) * kdim ** (-0.5)
    weight = weight.transpose(0, 2, 1).reshape(size * sub, heads, 1)
    scaled = key_cache.reshape(size * sub, heads, kdim).astype(jnp.float32) * weight
    kept = value_cache.reshape(size * sub, heads, vdim).astype(jnp.float32)
    memory = jnp.einsum("lhd,lhe->hde", scaled, kept, precision=HIGH)
    normal = jnp.sum(scaled, axis=0).reshape(pieces, 1, rows)
    fill = jnp.zeros((pieces, 6, vdim), jnp.float32)
    tail = jnp.pad(normal, ((0, 0), (0, 0), (0, vdim - rows)))
    level = jnp.broadcast_to(jnp.pad(stabilizer, (0, vdim - heads)) / pieces, (pieces, 1, vdim))
    share = jnp.concatenate([memory.reshape(pieces, rows, vdim), tail, level, fill], axis=1)
    groups = [[s * pieces + b for b in range(pieces)] for s in range(seqs)]
    share = lax.all_to_all(share, "sp", split_axis=0, concat_axis=0, tiled=True, axis_index_groups=groups)
    share = jnp.sum(share, axis=0)
    every = lax.all_gather(share, "sp").reshape(seqs, pieces, rows + 8, vdim)
    memory = every[:, :, :rows].reshape(seqs, heads, kdim, vdim)
    normalizer = every[:, :, rows, :rows].reshape(seqs, heads, kdim)
    stabilizer = every[:, 0, rows + 1, :heads]
    asked = query.astype(jnp.float32).reshape(seqs, heads, kdim)
    numer = jnp.sum(asked[..., None] * memory, axis=2)
    denom = jnp.maximum(jnp.abs(jnp.sum(asked * normalizer, axis=-1)), 1.0)
    first_read = (numer / denom[..., None]).reshape(seqs, heads * vdim)
    return (key_cache, value_cache, memory, normalizer, stabilizer, first_read)


def kernel(
    dims, tok, kw, vw, gw, bias, query,
    key_out, val_out, mem_out, norm_out, stab_out, read_out,
    key_send, val_send, gate_send, gate_got, wide, part, part_got, every,
    ks, kr, vs, vr, gs, gr, ps, pr, es, fs, er,
):
    seqs, span, heads, kdim, vdim, size = dims
    pieces = size // seqs
    sub = span // pieces
    rows = heads * kdim // pieces
    me = lax.axis_index("sp")
    seq, piece = me // pieces, me % pieces

    def copy(src, dst, send, recv, to):
        return pltpu.make_async_remote_copy(
            src_ref=src, dst_ref=dst, send_sem=send, recv_sem=recv,
            device_id={"sp": to}, device_id_type=pl.DeviceIdType.MESH,
        )

    barrier = pltpu.get_barrier_semaphore()
    for k in range(1, size):
        pl.semaphore_signal(
            barrier, inc=1, device_id={"sp": (me + k) % size}, device_id_type=pl.DeviceIdType.MESH
        )
    gates = lax.dot_general(
        tok[...], gw[...], (((1,), (1,)), ((), ())), preferred_element_type=jnp.float32
    ).T
    fpre = gates[heads : 2 * heads] + bias[...]
    logf = jnp.minimum(fpre, 0.0) - jnp.log1p(jnp.exp(-jnp.abs(fpre)))
    for s in range(seqs):
        gate_send[s, 0:heads, :] = gates[0:heads, s * span : (s + 1) * span]
        gate_send[s, heads : 2 * heads, :] = logf[:, s * span : (s + 1) * span]
    pl.semaphore_wait(barrier, size - 1)

    def gate_copy(k):
        to = (me + k) % size
        return copy(gate_send.at[to // pieces], gate_got.at[me], gs.at[to], gr.at[me], to)

    half = seqs // 2
    up = seq // half

    def key_copy(to):
        return copy(key_send.at[to], key_out.at[me], ks.at[to], kr.at[me], to)

    def val_copy(to):
        return copy(val_send.at[to], val_out.at[me], vs.at[to], vr.at[me], to)

    def project(k):
        off = up * ((k + 1) % seqs) + (1 - up) * (seqs - 1 - k)
        s = (seq + off) % seqs
        block = tok[pl.ds(pl.multiple_of(s * span, span), span), :]
        keys = jnp.dot(block, kw[...], preferred_element_type=jnp.float32).astype(jnp.bfloat16)
        for b in range(pieces):
            key_send[s * pieces + b] = keys[b * sub : (b + 1) * sub]
        values = jnp.dot(block, vw[...], preferred_element_type=jnp.float32).astype(jnp.bfloat16)
        for b in range(pieces):
            val_send[s * pieces + b] = values[b * sub : (b + 1) * sub]
        return s

    def step(k, carry):
        s = project(k)
        for b in range(pieces):
            key_copy(s * pieces + b).start()
            val_copy(s * pieces + b).start()
        return carry

    for k in range(1, size):
        gate_copy(k).start()
    lax.fori_loop(0, seqs - 1, step, 0)
    project(seqs - 1)
    for j in range(1, pieces):
        to = seq * pieces + (piece + j) % pieces
        key_copy(to).start()
        val_copy(to).start()
    key_out[me] = key_send[me]
    val_out[me] = val_send[me]
    gate_got[me] = gate_send[seq]

    for k in range(1, size):
        src = (me + k) % size
        copy(gate_send.at[seq], gate_got.at[src], gs.at[src], gr.at[src], src).wait_recv()
    got = gate_got[...]
    flat = got.reshape(size * 2 * heads, span)
    row = lax.broadcasted_iota(jnp.int32, (span, span), 0)
    col = lax.broadcasted_iota(jnp.int32, (span, span), 1)
    behind = jnp.where(row > col, 1.0, 0.0).astype(jnp.float32)
    after = jnp.dot(flat, behind, precision=HIGH, preferred_element_type=jnp.float32)
    after = after.reshape(size, 2 * heads, span)
    later = jnp.zeros((heads, 1), jnp.float32)
    logw = [None] * size
    for p in range(size - 1, -1, -1):
        logw[p] = after[p, heads:] + later + got[p, :heads]
        later = later + jnp.sum(got[p, heads:], axis=1, keepdims=True)
    top = functools.reduce(jnp.maximum, logw)
    stab = jnp.maximum(later, jnp.max(top, axis=1, keepdims=True))
    lane = lax.broadcasted_iota(jnp.int32, (2 * heads, heads * kdim), 1)
    head = lax.broadcasted_iota(jnp.int32, (2 * heads, heads * kdim), 0)
    spread = jnp.where((lane >= head * kdim) & (lane < (head + 1) * kdim), 1.0, 0.0).astype(jnp.float32)
    for p in range(size):
        weight = jnp.exp(logw[p] - stab) * kdim ** (-0.5)
        mine = weight[:, 0:sub]
        for b in range(1, pieces):
            mine = jnp.where(piece == b, weight[:, b * sub : (b + 1) * sub], mine)
        mine = jnp.concatenate([mine, jnp.zeros_like(mine)], axis=0).T
        wide[p] = jnp.dot(mine, spread, precision=HIGH, preferred_element_type=jnp.float32)

    for k in range(1, size):
        src = (me + k) % size
        copy(key_send.at[src], key_out.at[src], ks.at[src], kr.at[src], src).wait_recv()
        copy(val_send.at[src], val_out.at[src], vs.at[src], vr.at[src], src).wait_recv()
    scaled = key_out[...].astype(jnp.float32) * wide[...]
    scaled = scaled.reshape(size * sub, heads * kdim)
    normal = jnp.sum(scaled, axis=0, keepdims=True)
    turned = scaled.T
    high = turned.astype(jnp.bfloat16)
    low = (turned - high.astype(jnp.float32)).astype(jnp.bfloat16)
    kept = val_out[...].reshape(size * sub, heads * vdim)
    cross = jnp.dot(high, kept, preferred_element_type=jnp.float32)
    cross = cross + jnp.dot(low, kept, preferred_element_type=jnp.float32)
    per = heads // pieces
    for h in range(heads):
        at = (h % per) * kdim
        part[h // per, at : at + kdim, :] = cross[h * kdim : (h + 1) * kdim, h * vdim : (h + 1) * vdim]
    for b in range(pieces):
        part[b, rows : rows + 8, 0:rows] = jnp.broadcast_to(normal[:, b * rows : (b + 1) * rows], (8, rows))
        part[b, rows + 8 : rows + 16, :] = jnp.zeros((8, vdim), jnp.float32)

    for j in range(1, pieces):
        other = (piece + j) % pieces
        to = seq * pieces + other
        copy(part.at[other], part_got.at[piece], ps.at[other], pr.at[piece], to).start()
    share = part[piece]
    for j in range(1, pieces):
        other = (piece + j) % pieces
        to = seq * pieces + other
        copy(part.at[other], part_got.at[other], ps.at[other], pr.at[other], to).wait_recv()
        share = share + part_got[other]
    every[me] = share
    every[me, rows + 8 : rows + 8 + heads, :] = jnp.broadcast_to(stab, (heads, vdim))

    def across(k):
        to = ((seq + k) % seqs) * pieces + piece
        return copy(every.at[me], every.at[me], es.at[k], er.at[me], to)

    def along(k, j):
        src = ((seq + k) % seqs) * pieces + piece
        to = seq * pieces + (piece + j) % pieces
        return copy(every.at[src], every.at[src], fs.at[k, j], er.at[src], to)

    def landed(src):
        copy(every.at[src], every.at[src], es.at[0], er.at[src], src).wait_recv()

    for k in range(1, seqs):
        across(k).start()
    for j in range(1, pieces):
        along(0, j).start()
    for k in range(1, seqs):
        landed(((seq + k) % seqs) * pieces + piece)
        for j in range(1, pieces):
            along(k, j).start()
    for k in range(seqs):
        for j in range(1, pieces):
            landed(((seq + k) % seqs) * pieces + (piece + j) % pieces)

    asked = query[...].astype(jnp.float32)
    select = spread[0:heads]
    for s in range(seqs):
        for b in range(pieces):
            mem_out[s, b * rows : (b + 1) * rows, :] = every[s * pieces + b, 0:rows, :]
            norm_out[s : s + 1, b * rows : (b + 1) * rows] = every[s * pieces + b, rows : rows + 1, 0:rows]
        stab_out[s] = every[s * pieces, rows + 8 : rows + 8 + heads, :]
        one = asked[s : s + 1] * select
        numer = jnp.dot(one, mem_out[s], precision=HIGH, preferred_element_type=jnp.float32)
        inner = jnp.sum(one * norm_out[s : s + 1, :], axis=1, keepdims=True)
        read = numer / jnp.maximum(jnp.abs(inner), 1.0)
        for h in range(heads):
            read_out[s : s + 1, h * vdim : (h + 1) * vdim] = read[h : h + 1]

    for k in range(1, size):
        gate_copy(k).wait_send()
        key_copy((me + k) % size).wait_send()
        val_copy((me + k) % size).wait_send()
    for j in range(1, pieces):
        other = (piece + j) % pieces
        copy(part.at[other], part_got.at[piece], ps.at[other], pr.at[piece], seq * pieces + other).wait_send()
    for k in range(1, seqs):
        across(k).wait_send()
    for k in range(seqs):
        for j in range(1, pieces):
            along(k, j).wait_send()


def local(tokens, key_weight, value_weight, input_weight, forget_weight, forget_bias, query):
    seqs, span, width = tokens.shape
    heads = input_weight.shape[1]
    kdim = key_weight.shape[1] // heads
    vdim = value_weight.shape[1] // heads
    size = lax.axis_size("sp")
    pieces = size // seqs
    sub = span // pieces
    rows = heads * kdim // pieces
    fits = heads == 4 and pieces > 1 and heads % pieces == 0 and sub % 16 == 0 and seqs % 2 == 0
    if not fits or rows % 128 or rows > vdim or vdim % 128:
        return plain(tokens, key_weight, value_weight, input_weight, forget_weight, forget_bias, query)
    gates = jnp.concatenate([input_weight.T, forget_weight.T], axis=0)
    gates = jnp.pad(gates, ((0, 128 - 2 * heads), (0, 0)))
    f32, bf16 = jnp.float32, jnp.bfloat16
    vmem = pl.BlockSpec(memory_space=pltpu.VMEM)
    dma = pltpu.SemaphoreType.DMA
    outs = pl.pallas_call(
        functools.partial(kernel, (seqs, span, heads, kdim, vdim, size)),
        out_shape=(
            jax.ShapeDtypeStruct((size, sub, heads * kdim), bf16),
            jax.ShapeDtypeStruct((size, sub, heads * vdim), bf16),
            jax.ShapeDtypeStruct((seqs, heads * kdim, vdim), f32),
            jax.ShapeDtypeStruct((seqs, heads * kdim), f32),
            jax.ShapeDtypeStruct((seqs, heads, vdim), f32),
            jax.ShapeDtypeStruct((seqs, heads * vdim), f32),
        ),
        in_specs=[vmem] * 6,
        out_specs=(vmem,) * 6,
        scratch_shapes=[
            pltpu.VMEM((size, sub, heads * kdim), bf16),
            pltpu.VMEM((size, sub, heads * vdim), bf16),
            pltpu.VMEM((seqs, 2 * heads, span), f32),
            pltpu.VMEM((size, 2 * heads, span), f32),
            pltpu.VMEM((size, sub, heads * kdim), f32),
            pltpu.VMEM((pieces, rows + 16, vdim), f32),
            pltpu.VMEM((pieces, rows + 16, vdim), f32),
            pltpu.VMEM((size, rows + 16, vdim), f32),
            dma((size,)), dma((size,)), dma((size,)), dma((size,)), dma((size,)), dma((size,)),
            dma((pieces,)), dma((pieces,)), dma((seqs,)), dma((seqs, pieces)), dma((size,)),
        ],
        compiler_params=pltpu.CompilerParams(
            collective_id=0, has_side_effects=True, vmem_limit_bytes=48 * 1024 * 1024
        ),
    )(tokens.reshape(seqs * span, width), key_weight, value_weight, gates, forget_bias[:, None], query)
    keys, values, memory, normalizer, level, first_read = outs
    return (
        keys.reshape(1, size * sub, heads * kdim),
        values.reshape(1, size * sub, heads * vdim),
        memory.reshape(seqs, heads, kdim, vdim),
        normalizer.reshape(seqs, heads, kdim),
        level[:, :, 0],
        first_read,
    )


def solution(mesh):
    return jax.shard_map(
        local,
        mesh=mesh,
        in_specs=(
            P("gr", "sp", None),
            P(None, "tp"),
            P(None, "tp"),
            P(None, "tp"),
            P(None, "tp"),
            P("tp"),
            P("gr", "tp"),
        ),
        out_specs=(
            P(("gr", "sp"), None, "tp"),
            P(("gr", "sp"), None, "tp"),
            P("gr", "tp", None, None),
            P("gr", "tp", None),
            P("gr", "tp"),
            P("gr", "tp"),
        ),
        check_vma=False,
    )
```

```python
import functools

import jax
import jax.numpy as jnp
from jax import lax
from jax.experimental import pallas as pl
from jax.experimental.pallas import tpu as pltpu
from jax.sharding import PartitionSpec as P

HIGH = lax.Precision.HIGHEST


def plain(tokens, key_weight, value_weight, input_weight, forget_weight, forget_bias, query):
    seqs, span, width = tokens.shape
    heads = input_weight.shape[1]
    kdim = key_weight.shape[1] // heads
    vdim = value_weight.shape[1] // heads
    size = lax.axis_size("sp")
    me = lax.axis_index("sp")
    pieces = size // seqs
    sub = span // pieces
    rows = heads * kdim // pieces
    flat = tokens.reshape(seqs * span, width)
    gate_pair = jnp.concatenate([input_weight, forget_weight], axis=1)
    gates = lax.dot_general(gate_pair, flat, (((0,), (1,)), ((), ())), preferred_element_type=jnp.float32)
    igate = gates[:heads]
    logf = jax.nn.log_sigmoid(gates[heads:] + forget_bias[:, None])
    packet = jnp.concatenate([igate, logf]).reshape(2 * heads, seqs, span).transpose(1, 0, 2)
    packet = jnp.repeat(packet, pieces, axis=0)
    packet = lax.all_to_all(packet, "sp", split_axis=0, concat_axis=0, tiled=True)
    values = jnp.dot(flat, value_weight, preferred_element_type=jnp.float32).astype(jnp.bfloat16)
    keys = jnp.dot(flat, key_weight, preferred_element_type=jnp.float32).astype(jnp.bfloat16)
    value_cache = lax.all_to_all(
        values.reshape(size, sub, heads * vdim), "sp", split_axis=0, concat_axis=1, tiled=True
    )
    key_cache = lax.all_to_all(
        keys.reshape(size, sub, heads * kdim), "sp", split_axis=0, concat_axis=1, tiled=True
    )
    igate, logf = packet[:, :heads], packet[:, heads:]
    at = jnp.arange(span)
    behind = (at[:, None] > at[None, :]).astype(jnp.float32)
    after = jnp.einsum("pht,ts->phs", logf, behind, precision=HIGH)
    sums = jnp.sum(logf, axis=2)
    block = jnp.arange(size)
    later = jnp.sum(jnp.where(block[:, None, None] > block[None, :, None], sums[:, None, :], 0.0), axis=0)
    total = jnp.sum(sums, axis=0)
    logw = after + later[:, :, None] + igate
    stabilizer = jnp.maximum(total, jnp.max(logw, axis=(0, 2)))
    mine = lax.dynamic_slice_in_dim(logw, lax.rem(me, pieces) * sub, sub, axis=2)
    weight = jnp.exp(mine - stabilizer[None, :, None]) * kdim ** (-0.5)
    weight = weight.transpose(0, 2, 1).reshape(size * sub, heads, 1)
    scaled = key_cache.reshape(size * sub, heads, kdim).astype(jnp.float32) * weight
    kept = value_cache.reshape(size * sub, heads, vdim).astype(jnp.float32)
    memory = jnp.einsum("lhd,lhe->hde", scaled, kept, precision=HIGH)
    normal = jnp.sum(scaled, axis=0).reshape(pieces, 1, rows)
    fill = jnp.zeros((pieces, 6, vdim), jnp.float32)
    tail = jnp.pad(normal, ((0, 0), (0, 0), (0, vdim - rows)))
    level = jnp.broadcast_to(jnp.pad(stabilizer, (0, vdim - heads)) / pieces, (pieces, 1, vdim))
    share = jnp.concatenate([memory.reshape(pieces, rows, vdim), tail, level, fill], axis=1)
    groups = [[s * pieces + b for b in range(pieces)] for s in range(seqs)]
    share = lax.all_to_all(share, "sp", split_axis=0, concat_axis=0, tiled=True, axis_index_groups=groups)
    share = jnp.sum(share, axis=0)
    every = lax.all_gather(share, "sp").reshape(seqs, pieces, rows + 8, vdim)
    memory = every[:, :, :rows].reshape(seqs, heads, kdim, vdim)
    normalizer = every[:, :, rows, :rows].reshape(seqs, heads, kdim)
    stabilizer = every[:, 0, rows + 1, :heads]
    asked = query.astype(jnp.float32).reshape(seqs, heads, kdim)
    numer = jnp.sum(asked[..., None] * memory, axis=2)
    denom = jnp.maximum(jnp.abs(jnp.sum(asked * normalizer, axis=-1)), 1.0)
    first_read = (numer / denom[..., None]).reshape(seqs, heads * vdim)
    return (key_cache, value_cache, memory, normalizer, stabilizer, first_read)


def kernel(
    dims, tok, kw, vw, gw, bias, query,
    key_hbm, val_hbm, mem_out, norm_out, stab_out, read_out,
    key_out, val_out, tokens, key_w, val_w, key_send, val_send, gate_send, gate_got, wide, cross, part, part_got, every,
    hs, ts, ws,
    ks, kr, vs, vr, gs, gr, ps, pr, es, fs, er,
):
    seqs, span, heads, kdim, vdim, size = dims
    pieces = size // seqs
    sub = span // pieces
    rows = heads * kdim // pieces
    me = lax.axis_index("sp")
    seq, piece = me // pieces, me % pieces

    def copy(src, dst, send, recv, to):
        return pltpu.make_async_remote_copy(
            src_ref=src, dst_ref=dst, send_sem=send, recv_sem=recv,
            device_id={"sp": to}, device_id_type=pl.DeviceIdType.MESH,
        )

    half = seqs // 2
    up = seq // half

    def turn(k):
        off = up * ((k + 1) % seqs) + (1 - up) * (seqs - 1 - k)
        return (seq + off) % seqs

    def load(k):
        at = pl.ds(pl.multiple_of(turn(k) * span, span), span)
        return pltpu.make_async_copy(tok.at[at], tokens.at[at], ts.at[k])

    key_load = pltpu.make_async_copy(kw, key_w, ws.at[0])
    val_load = pltpu.make_async_copy(vw, val_w, ws.at[1])
    load(0).start()
    key_load.start()
    val_load.start()
    for k in range(1, seqs):
        load(k).start()
    barrier = pltpu.get_barrier_semaphore()
    for k in range(1, size):
        pl.semaphore_signal(
            barrier, inc=1, device_id={"sp": (me + k) % size}, device_id_type=pl.DeviceIdType.MESH
        )
    pl.semaphore_wait(barrier, size - 1)

    def gate_copy(to):
        return copy(gate_send.at[to // pieces], gate_got.at[me], gs.at[to], gr.at[me], to)

    def key_copy(to):
        return copy(key_send.at[to], key_out.at[me], ks.at[to], kr.at[me], to)

    def val_copy(to):
        return copy(val_send.at[to], val_out.at[me], vs.at[to], vr.at[me], to)

    def project(k):
        s = turn(k)
        load(k).wait()
        block = tokens[pl.ds(pl.multiple_of(s * span, span), span), :]
        keys = jnp.dot(block, key_w[...], preferred_element_type=jnp.float32).astype(jnp.bfloat16)
        for b in range(pieces):
            key_send[s * pieces + b] = keys[b * sub : (b + 1) * sub]
        gates = lax.dot_general(
            block, gw[...], (((1,), (1,)), ((), ())), preferred_element_type=jnp.float32
        ).T
        fpre = gates[heads : 2 * heads] + bias[...]
        gate_send[s, 0:heads, :] = gates[0:heads]
        gate_send[s, heads : 2 * heads, :] = jnp.minimum(fpre, 0.0) - jnp.log1p(jnp.exp(-jnp.abs(fpre)))
        values = jnp.dot(block, val_w[...], preferred_element_type=jnp.float32).astype(jnp.bfloat16)
        for b in range(pieces):
            val_send[s * pieces + b] = values[b * sub : (b + 1) * sub]
        return s

    def step(k, carry):
        s = project(k)
        for b in range(pieces):
            gate_copy(s * pieces + b).start()
        for b in range(pieces):
            key_copy(s * pieces + b).start()
            val_copy(s * pieces + b).start()
        return carry

    key_load.wait()
    val_load.wait()
    lax.fori_loop(0, seqs - 1, step, 0)
    project(seqs - 1)
    for j in range(1, pieces):
        to = seq * pieces + (piece + j) % pieces
        gate_copy(to).start()
        key_copy(to).start()
        val_copy(to).start()
    key_out[me] = key_send[me]
    val_out[me] = val_send[me]
    gate_got[me] = gate_send[seq]

    for k in range(1, size):
        src = (me + k) % size
        copy(gate_send.at[seq], gate_got.at[src], gs.at[src], gr.at[src], src).wait_recv()
    got = gate_got[...]
    flat = got.reshape(size * 2 * heads, span)
    row = lax.broadcasted_iota(jnp.int32, (span, span), 0)
    col = lax.broadcasted_iota(jnp.int32, (span, span), 1)
    behind = jnp.where(row > col, 1.0, 0.0).astype(jnp.float32)
    after = jnp.dot(flat, behind, precision=HIGH, preferred_element_type=jnp.float32)
    after = after.reshape(size, 2 * heads, span)
    later = jnp.zeros((heads, 1), jnp.float32)
    logw = [None] * size
    for p in range(size - 1, -1, -1):
        logw[p] = after[p, heads:] + later + got[p, :heads]
        later = later + jnp.sum(got[p, heads:], axis=1, keepdims=True)
    top = functools.reduce(jnp.maximum, logw)
    stab = jnp.maximum(later, jnp.max(top, axis=1, keepdims=True))
    lane = lax.broadcasted_iota(jnp.int32, (2 * heads, heads * kdim), 1)
    head = lax.broadcasted_iota(jnp.int32, (2 * heads, heads * kdim), 0)
    spread = jnp.where((lane >= head * kdim) & (lane < (head + 1) * kdim), 1.0, 0.0).astype(jnp.float32)
    for p in range(size):
        weight = jnp.exp(logw[p] - stab) * kdim ** (-0.5)
        mine = weight[:, 0:sub]
        for b in range(1, pieces):
            mine = jnp.where(piece == b, weight[:, b * sub : (b + 1) * sub], mine)
        mine = jnp.concatenate([mine, jnp.zeros_like(mine)], axis=0).T
        wide[p] = jnp.dot(mine, spread, precision=HIGH, preferred_element_type=jnp.float32)

    normal = jnp.zeros((1, heads * kdim), jnp.float32)
    for k in range(seqs - 1, -1, -1):
        first = turn(k) * pieces
        for j in range(pieces):
            if k == seqs - 1 and j == 0:
                continue
            src = first + (piece + j) % pieces
            copy(key_send.at[src], key_out.at[src], ks.at[src], kr.at[src], src).wait_recv()
            copy(val_send.at[src], val_out.at[src], vs.at[src], vr.at[src], src).wait_recv()
        group = pl.ds(first, pieces)
        scaled = key_out[group].astype(jnp.float32) * wide[group]
        scaled = scaled.reshape(span, heads * kdim)
        normal = normal + jnp.sum(scaled, axis=0, keepdims=True)
        turned = scaled.T
        high = turned.astype(jnp.bfloat16)
        low = (turned - high.astype(jnp.float32)).astype(jnp.bfloat16)
        kept = val_out[group].reshape(span, heads * vdim)
        term = jnp.dot(high, kept, preferred_element_type=jnp.float32)
        term = term + jnp.dot(low, kept, preferred_element_type=jnp.float32)
        cross[...] = term if k == seqs - 1 else cross[...] + term
    keep = (
        pltpu.make_async_copy(key_out, key_hbm, hs.at[0]),
        pltpu.make_async_copy(val_out, val_hbm, hs.at[1]),
    )
    for one in keep:
        one.start()
    per = heads // pieces
    for h in range(heads):
        at = (h % per) * kdim
        part[h // per, at : at + kdim, :] = cross[h * kdim : (h + 1) * kdim, h * vdim : (h + 1) * vdim]
    for b in range(pieces):
        part[b, rows : rows + 8, 0:rows] = jnp.broadcast_to(normal[:, b * rows : (b + 1) * rows], (8, rows))
        part[b, rows + 8 : rows + 16, :] = jnp.zeros((8, vdim), jnp.float32)

    for j in range(1, pieces):
        other = (piece + j) % pieces
        to = seq * pieces + other
        copy(part.at[other], part_got.at[piece], ps.at[other], pr.at[piece], to).start()
    share = part[piece]
    for j in range(1, pieces):
        other = (piece + j) % pieces
        to = seq * pieces + other
        copy(part.at[other], part_got.at[other], ps.at[other], pr.at[other], to).wait_recv()
        share = share + part_got[other]
    every[me] = share
    every[me, rows + 8 : rows + 8 + heads, :] = jnp.broadcast_to(stab, (heads, vdim))

    def across(k):
        to = ((seq + k) % seqs) * pieces + piece
        return copy(every.at[me], every.at[me], es.at[k], er.at[me], to)

    def along(k, j):
        src = ((seq + k) % seqs) * pieces + piece
        to = seq * pieces + (piece + j) % pieces
        return copy(every.at[src], every.at[src], fs.at[k, j], er.at[src], to)

    def landed(src):
        copy(every.at[src], every.at[src], es.at[0], er.at[src], src).wait_recv()

    for k in range(1, seqs):
        across(k).start()
    for j in range(1, pieces):
        along(0, j).start()
    for k in range(1, seqs):
        landed(((seq + k) % seqs) * pieces + piece)
        for j in range(1, pieces):
            along(k, j).start()
    for k in range(seqs):
        for j in range(1, pieces):
            landed(((seq + k) % seqs) * pieces + (piece + j) % pieces)

    asked = query[...].astype(jnp.float32)
    select = spread[0:heads]
    wide_row = lax.broadcasted_iota(jnp.int32, (heads, vdim), 0)
    diagonal = lax.broadcasted_iota(jnp.int32, (heads, vdim), 1) == wide_row
    for s in range(seqs):
        for b in range(pieces):
            mem_out[s, b * rows : (b + 1) * rows, :] = every[s * pieces + b, 0:rows, :]
        level = every[s * pieces, rows + 8 : rows + 8 + heads, :]
        level = jnp.sum(jnp.where(diagonal, level, 0.0), axis=0, keepdims=True)
        stab_out[s : s + 1, :] = level[:, 0:heads]
        normal = jnp.concatenate([every[s * pieces + b, rows : rows + 1, 0:rows] for b in range(pieces)], axis=1)
        for h in range(heads):
            norm_out[s, h : h + 1, :] = normal[:, h * kdim : (h + 1) * kdim]
        picked = asked[s : s + 1] * select
        numer = jnp.dot(picked, mem_out[s], precision=HIGH, preferred_element_type=jnp.float32)
        inner = jnp.sum(picked * normal, axis=1, keepdims=True)
        read = numer / jnp.maximum(jnp.abs(inner), 1.0)
        for h in range(heads):
            read_out[s : s + 1, h * vdim : (h + 1) * vdim] = read[h : h + 1]

    for one in keep:
        one.wait()
    for k in range(1, size):
        gate_copy((me + k) % size).wait_send()
        key_copy((me + k) % size).wait_send()
        val_copy((me + k) % size).wait_send()
    for j in range(1, pieces):
        other = (piece + j) % pieces
        copy(part.at[other], part_got.at[piece], ps.at[other], pr.at[piece], seq * pieces + other).wait_send()
    for k in range(1, seqs):
        across(k).wait_send()
    for k in range(seqs):
        for j in range(1, pieces):
            along(k, j).wait_send()


def write_out(k_in, v_in, m_in, n_in, s_in, r_in, k_out, v_out, m_out, n_out, s_out, r_out, kb, vb, mb, reads, writes):
    chain = ((v_in, vb, v_out), (m_in, mb, m_out), (k_in, kb, k_out))
    ins = [pltpu.make_async_copy(a, b, reads.at[i]) for i, (a, b, c) in enumerate(chain)]
    outs = [pltpu.make_async_copy(b, c, writes.at[i]) for i, (a, b, c) in enumerate(chain)]
    for one in ins:
        one.start()
    n_out[...] = n_in[...]
    s_out[...] = s_in[...]
    r_out[...] = r_in[...]
    for first, then in zip(ins, outs):
        first.wait()
        then.start()
    for one in outs:
        one.wait()


def local(tokens, key_weight, value_weight, input_weight, forget_weight, forget_bias, query):
    seqs, span, width = tokens.shape
    heads = input_weight.shape[1]
    kdim = key_weight.shape[1] // heads
    vdim = value_weight.shape[1] // heads
    size = lax.axis_size("sp")
    pieces = size // seqs
    sub = span // pieces
    rows = heads * kdim // pieces
    fits = heads == 4 and pieces > 1 and heads % pieces == 0 and sub % 16 == 0 and seqs % 2 == 0
    if not fits or rows % 128 or rows > vdim or vdim % 128:
        return plain(tokens, key_weight, value_weight, input_weight, forget_weight, forget_bias, query)
    gates = jnp.concatenate([input_weight.T, forget_weight.T], axis=0)
    gates = jnp.pad(gates, ((0, 8 * heads - 2 * heads), (0, 0)))
    f32, bf16 = jnp.float32, jnp.bfloat16
    vmem = pl.BlockSpec(memory_space=pltpu.VMEM)
    hbm = pl.BlockSpec(memory_space=pltpu.HBM)
    dma = pltpu.SemaphoreType.DMA
    outs = pl.pallas_call(
        functools.partial(kernel, (seqs, span, heads, kdim, vdim, size)),
        out_shape=(
            jax.ShapeDtypeStruct((size, sub, heads * kdim), bf16),
            jax.ShapeDtypeStruct((size, sub, heads * vdim), bf16),
            jax.ShapeDtypeStruct((seqs, heads * kdim, vdim), f32),
            jax.ShapeDtypeStruct((seqs, heads, kdim), f32),
            jax.ShapeDtypeStruct((seqs, heads), f32),
            jax.ShapeDtypeStruct((seqs, heads * vdim), f32),
        ),
        in_specs=[hbm] * 3 + [vmem] * 3,
        out_specs=(hbm,) * 2 + (vmem,) * 4,
        scratch_shapes=[
            pltpu.VMEM((size, sub, heads * kdim), bf16),
            pltpu.VMEM((size, sub, heads * vdim), bf16),
            pltpu.VMEM((seqs * span, width), bf16),
            pltpu.VMEM(key_weight.shape, bf16),
            pltpu.VMEM(value_weight.shape, bf16),
            pltpu.VMEM((size, sub, heads * kdim), bf16),
            pltpu.VMEM((size, sub, heads * vdim), bf16),
            pltpu.VMEM((seqs, 2 * heads, span), f32),
            pltpu.VMEM((size, 2 * heads, span), f32),
            pltpu.VMEM((size, sub, heads * kdim), f32),
            pltpu.VMEM((heads * kdim, heads * vdim), f32),
            pltpu.VMEM((pieces, rows + 16, vdim), f32),
            pltpu.VMEM((pieces, rows + 16, vdim), f32),
            pltpu.VMEM((size, rows + 16, vdim), f32),
            dma((2,)), dma((seqs,)), dma((2,)),
            dma((size,)), dma((size,)), dma((size,)), dma((size,)), dma((size,)), dma((size,)),
            dma((pieces,)), dma((pieces,)), dma((seqs,)), dma((seqs, pieces)), dma((size,)),
        ],
        compiler_params=pltpu.CompilerParams(
            collective_id=0, has_side_effects=True, vmem_limit_bytes=63 * 1024 * 1024
        ),
    )(tokens.reshape(seqs * span, width), key_weight, value_weight, gates, forget_bias[:, None], query)
    outs = pl.pallas_call(
        write_out,
        out_shape=tuple(jax.ShapeDtypeStruct(x.shape, x.dtype) for x in outs),
        in_specs=[hbm] * 3 + [vmem] * 3,
        out_specs=(hbm,) * 3 + (vmem,) * 3,
        scratch_shapes=[pltpu.VMEM(x.shape, x.dtype) for x in (outs[0], outs[1], outs[2])]
        + [dma((3,)), dma((3,))],
        compiler_params=pltpu.CompilerParams(vmem_limit_bytes=63 * 1024 * 1024),
    )(*outs)
    keys, values, memory, normalizer, stabilizer, first_read = outs
    return (
        keys.reshape(1, size * sub, heads * kdim),
        values.reshape(1, size * sub, heads * vdim),
        memory.reshape(seqs, heads, kdim, vdim),
        normalizer,
        stabilizer,
        first_read,
    )


def solution(mesh):
    return jax.shard_map(
        local,
        mesh=mesh,
        in_specs=(
            P("gr", "sp", None),
            P(None, "tp"),
            P(None, "tp"),
            P(None, "tp"),
            P(None, "tp"),
            P("tp"),
            P("gr", "tp"),
        ),
        out_specs=(
            P(("gr", "sp"), None, "tp"),
            P(("gr", "sp"), None, "tp"),
            P("gr", "tp", None, None),
            P("gr", "tp", None),
            P("gr", "tp"),
            P("gr", "tp"),
        ),
        check_vma=False,
    )
```

```python
import functools

import jax
import jax.numpy as jnp
from jax import lax
from jax.experimental import pallas as pl
from jax.experimental.pallas import tpu as pltpu
from jax.sharding import PartitionSpec as P

HIGH = lax.Precision.HIGHEST


def plain(tokens, key_weight, value_weight, input_weight, forget_weight, forget_bias, query):
    seqs, span, width = tokens.shape
    heads = input_weight.shape[1]
    kdim = key_weight.shape[1] // heads
    vdim = value_weight.shape[1] // heads
    size = lax.axis_size("sp")
    me = lax.axis_index("sp")
    pieces = size // seqs
    sub = span // pieces
    rows = heads * kdim // pieces
    flat = tokens.reshape(seqs * span, width)
    gate_pair = jnp.concatenate([input_weight, forget_weight], axis=1)
    gates = lax.dot_general(gate_pair, flat, (((0,), (1,)), ((), ())), preferred_element_type=jnp.float32)
    igate = gates[:heads]
    logf = jax.nn.log_sigmoid(gates[heads:] + forget_bias[:, None])
    packet = jnp.concatenate([igate, logf]).reshape(2 * heads, seqs, span).transpose(1, 0, 2)
    packet = jnp.repeat(packet, pieces, axis=0)
    packet = lax.all_to_all(packet, "sp", split_axis=0, concat_axis=0, tiled=True)
    values = jnp.dot(flat, value_weight, preferred_element_type=jnp.float32).astype(jnp.bfloat16)
    keys = jnp.dot(flat, key_weight, preferred_element_type=jnp.float32).astype(jnp.bfloat16)
    value_cache = lax.all_to_all(
        values.reshape(size, sub, heads * vdim), "sp", split_axis=0, concat_axis=1, tiled=True
    )
    key_cache = lax.all_to_all(
        keys.reshape(size, sub, heads * kdim), "sp", split_axis=0, concat_axis=1, tiled=True
    )
    igate, logf = packet[:, :heads], packet[:, heads:]
    at = jnp.arange(span)
    behind = (at[:, None] > at[None, :]).astype(jnp.float32)
    after = jnp.einsum("pht,ts->phs", logf, behind, precision=HIGH)
    sums = jnp.sum(logf, axis=2)
    block = jnp.arange(size)
    later = jnp.sum(jnp.where(block[:, None, None] > block[None, :, None], sums[:, None, :], 0.0), axis=0)
    total = jnp.sum(sums, axis=0)
    logw = after + later[:, :, None] + igate
    stabilizer = jnp.maximum(total, jnp.max(logw, axis=(0, 2)))
    mine = lax.dynamic_slice_in_dim(logw, lax.rem(me, pieces) * sub, sub, axis=2)
    weight = jnp.exp(mine - stabilizer[None, :, None]) * kdim ** (-0.5)
    weight = weight.transpose(0, 2, 1).reshape(size * sub, heads, 1)
    scaled = key_cache.reshape(size * sub, heads, kdim).astype(jnp.float32) * weight
    kept = value_cache.reshape(size * sub, heads, vdim).astype(jnp.float32)
    memory = jnp.einsum("lhd,lhe->hde", scaled, kept, precision=HIGH)
    normal = jnp.sum(scaled, axis=0).reshape(pieces, 1, rows)
    fill = jnp.zeros((pieces, 6, vdim), jnp.float32)
    tail = jnp.pad(normal, ((0, 0), (0, 0), (0, vdim - rows)))
    level = jnp.broadcast_to(jnp.pad(stabilizer, (0, vdim - heads)) / pieces, (pieces, 1, vdim))
    share = jnp.concatenate([memory.reshape(pieces, rows, vdim), tail, level, fill], axis=1)
    groups = [[s * pieces + b for b in range(pieces)] for s in range(seqs)]
    share = lax.all_to_all(share, "sp", split_axis=0, concat_axis=0, tiled=True, axis_index_groups=groups)
    share = jnp.sum(share, axis=0)
    every = lax.all_gather(share, "sp").reshape(seqs, pieces, rows + 8, vdim)
    memory = every[:, :, :rows].reshape(seqs, heads, kdim, vdim)
    normalizer = every[:, :, rows, :rows].reshape(seqs, heads, kdim)
    stabilizer = every[:, 0, rows + 1, :heads]
    asked = query.astype(jnp.float32).reshape(seqs, heads, kdim)
    numer = jnp.sum(asked[..., None] * memory, axis=2)
    denom = jnp.maximum(jnp.abs(jnp.sum(asked * normalizer, axis=-1)), 1.0)
    first_read = (numer / denom[..., None]).reshape(seqs, heads * vdim)
    return (key_cache, value_cache, memory, normalizer, stabilizer, first_read)


def kernel(
    dims, tok, kw, vw, gw, bias, query,
    key_hbm, val_hbm, mem_out, norm_out, stab_out, read_out,
    key_out, val_out, tokens, key_w, val_w, key_send, val_send, gate_send, gate_got, wide, cross, part, part_got, every,
    hs, ts, ws,
    ks, kr, vs, vr, gs, gr, ps, pr, es, fs, er,
):
    seqs, span, heads, kdim, vdim, size = dims
    pieces = size // seqs
    sub = span // pieces
    rows = heads * kdim // pieces
    me = lax.axis_index("sp")
    seq, piece = me // pieces, me % pieces

    def copy(src, dst, send, recv, to):
        return pltpu.make_async_remote_copy(
            src_ref=src, dst_ref=dst, send_sem=send, recv_sem=recv,
            device_id={"sp": to}, device_id_type=pl.DeviceIdType.MESH,
        )

    half = seqs // 2
    up = seq // half

    def turn(k):
        off = up * ((k + 1) % seqs) + (1 - up) * (seqs - 1 - k)
        return (seq + off) % seqs

    def load(k):
        at = pl.ds(pl.multiple_of(turn(k) * span, span), span)
        return pltpu.make_async_copy(tok.at[at], tokens.at[at], ts.at[k])

    key_load = pltpu.make_async_copy(kw, key_w, ws.at[0])
    val_load = pltpu.make_async_copy(vw, val_w, ws.at[1])
    load(0).start()
    key_load.start()
    val_load.start()
    for k in range(1, seqs):
        load(k).start()
    barrier = pltpu.get_barrier_semaphore()
    for k in range(1, size):
        pl.semaphore_signal(
            barrier, inc=1, device_id={"sp": (me + k) % size}, device_id_type=pl.DeviceIdType.MESH
        )
    pl.semaphore_wait(barrier, size - 1)

    def gate_copy(to):
        return copy(gate_send.at[to // pieces], gate_got.at[me], gs.at[to], gr.at[me], to)

    def key_copy(to):
        return copy(key_send.at[to], key_out.at[me], ks.at[to], kr.at[me], to)

    def val_copy(to):
        return copy(val_send.at[to], val_out.at[me], vs.at[to], vr.at[me], to)

    def project(k):
        s = turn(k)
        block = tokens[pl.ds(pl.multiple_of(s * span, span), span), :]
        keys = jnp.dot(block, key_w[...], preferred_element_type=jnp.float32).astype(jnp.bfloat16)
        for b in range(pieces):
            key_send[s * pieces + b] = keys[b * sub : (b + 1) * sub]
        values = jnp.dot(block, val_w[...], preferred_element_type=jnp.float32).astype(jnp.bfloat16)
        for b in range(pieces):
            val_send[s * pieces + b] = values[b * sub : (b + 1) * sub]
        return s

    def step(k, carry):
        s = project(k)
        for b in range(pieces):
            key_copy(s * pieces + b).start()
            val_copy(s * pieces + b).start()
        return carry

    key_load.wait()
    val_load.wait()
    load(0).wait()
    step(0, 0)
    for k in range(1, seqs):
        load(k).wait()
    gates = lax.dot_general(
        tokens[...], gw[...], (((1,), (1,)), ((), ())), preferred_element_type=jnp.float32
    ).T
    own = lax.broadcasted_iota(jnp.int32, (heads, heads), 0) == lax.broadcasted_iota(jnp.int32, (heads, heads), 1)
    shift = jnp.sum(jnp.where(own, jnp.broadcast_to(bias[...], (heads, heads)), 0.0), axis=1, keepdims=True)
    fpre = gates[heads : 2 * heads] + shift
    logf = jnp.minimum(fpre, 0.0) - jnp.log1p(jnp.exp(-jnp.abs(fpre)))
    for s in range(seqs):
        gate_send[s, 0:heads, :] = gates[0:heads, s * span : (s + 1) * span]
        gate_send[s, heads : 2 * heads, :] = logf[:, s * span : (s + 1) * span]
    for k in range(1, size):
        gate_copy((me + k) % size).start()
    lax.fori_loop(1, seqs - 1, step, 0)
    project(seqs - 1)
    for j in range(1, pieces):
        to = seq * pieces + (piece + j) % pieces
        key_copy(to).start()
        val_copy(to).start()
    key_out[me] = key_send[me]
    val_out[me] = val_send[me]
    gate_got[me] = gate_send[seq]

    for k in range(1, size):
        src = (me + k) % size
        copy(gate_send.at[seq], gate_got.at[src], gs.at[src], gr.at[src], src).wait_recv()
    got = gate_got[...]
    flat = got.reshape(size * 2 * heads, span)
    row = lax.broadcasted_iota(jnp.int32, (span, span), 0)
    col = lax.broadcasted_iota(jnp.int32, (span, span), 1)
    behind = jnp.where(row > col, 1.0, 0.0).astype(jnp.float32)
    after = jnp.dot(flat, behind, precision=HIGH, preferred_element_type=jnp.float32)
    after = after.reshape(size, 2 * heads, span)
    later = jnp.zeros((heads, 1), jnp.float32)
    logw = [None] * size
    for p in range(size - 1, -1, -1):
        logw[p] = after[p, heads:] + later + got[p, :heads]
        later = later + jnp.sum(got[p, heads:], axis=1, keepdims=True)
    top = functools.reduce(jnp.maximum, logw)
    stab = jnp.maximum(later, jnp.max(top, axis=1, keepdims=True))
    lane = lax.broadcasted_iota(jnp.int32, (2 * heads, heads * kdim), 1)
    head = lax.broadcasted_iota(jnp.int32, (2 * heads, heads * kdim), 0)
    spread = jnp.where((lane >= head * kdim) & (lane < (head + 1) * kdim), 1.0, 0.0).astype(jnp.float32)
    for p in range(size):
        weight = jnp.exp(logw[p] - stab) * kdim ** (-0.5)
        mine = weight[:, 0:sub]
        for b in range(1, pieces):
            mine = jnp.where(piece == b, weight[:, b * sub : (b + 1) * sub], mine)
        mine = jnp.concatenate([mine, jnp.zeros_like(mine)], axis=0).T
        wide[p] = jnp.dot(mine, spread, precision=HIGH, preferred_element_type=jnp.float32)

    normal = jnp.zeros((1, heads * kdim), jnp.float32)
    for k in range(seqs - 1, -1, -1):
        first = turn(k) * pieces
        for j in range(pieces):
            if k == seqs - 1 and j == 0:
                continue
            src = first + (piece + j) % pieces
            copy(key_send.at[src], key_out.at[src], ks.at[src], kr.at[src], src).wait_recv()
            copy(val_send.at[src], val_out.at[src], vs.at[src], vr.at[src], src).wait_recv()
        group = pl.ds(first, pieces)
        scaled = key_out[group].astype(jnp.float32) * wide[group]
        scaled = scaled.reshape(span, heads * kdim)
        normal = normal + jnp.sum(scaled, axis=0, keepdims=True)
        turned = scaled.T
        high = turned.astype(jnp.bfloat16)
        low = (turned - high.astype(jnp.float32)).astype(jnp.bfloat16)
        kept = val_out[group].reshape(span, heads * vdim)
        term = jnp.dot(high, kept, preferred_element_type=jnp.float32)
        term = term + jnp.dot(low, kept, preferred_element_type=jnp.float32)
        cross[...] = term if k == seqs - 1 else cross[...] + term
    keep = (
        pltpu.make_async_copy(key_out, key_hbm, hs.at[0]),
        pltpu.make_async_copy(val_out, val_hbm, hs.at[1]),
    )
    for one in keep:
        one.start()
    per = heads // pieces
    for h in range(heads):
        at = (h % per) * kdim
        part[h // per, at : at + kdim, :] = cross[h * kdim : (h + 1) * kdim, h * vdim : (h + 1) * vdim]
    for b in range(pieces):
        part[b, rows : rows + 8, 0:rows] = jnp.broadcast_to(normal[:, b * rows : (b + 1) * rows], (8, rows))
        part[b, rows + 8 : rows + 16, :] = jnp.zeros((8, vdim), jnp.float32)

    for j in range(1, pieces):
        other = (piece + j) % pieces
        to = seq * pieces + other
        copy(part.at[other], part_got.at[piece], ps.at[other], pr.at[piece], to).start()
    share = part[piece]
    for j in range(1, pieces):
        other = (piece + j) % pieces
        to = seq * pieces + other
        copy(part.at[other], part_got.at[other], ps.at[other], pr.at[other], to).wait_recv()
        share = share + part_got[other]
    every[me] = share
    every[me, rows + 8 : rows + 8 + heads, :] = jnp.broadcast_to(stab, (heads, vdim))

    def across(k):
        to = ((seq + k) % seqs) * pieces + piece
        return copy(every.at[me], every.at[me], es.at[k], er.at[me], to)

    def along(k, j):
        src = ((seq + k) % seqs) * pieces + piece
        to = seq * pieces + (piece + j) % pieces
        return copy(every.at[src], every.at[src], fs.at[k, j], er.at[src], to)

    def landed(src):
        copy(every.at[src], every.at[src], es.at[0], er.at[src], src).wait_recv()

    for k in range(1, seqs):
        across(k).start()
    for j in range(1, pieces):
        along(0, j).start()
    for k in range(1, seqs):
        landed(((seq + k) % seqs) * pieces + piece)
        for j in range(1, pieces):
            along(k, j).start()
    for k in range(seqs):
        for j in range(1, pieces):
            landed(((seq + k) % seqs) * pieces + (piece + j) % pieces)

    asked = query[...].astype(jnp.float32)
    select = spread[0:heads]
    wide_row = lax.broadcasted_iota(jnp.int32, (heads, vdim), 0)
    diagonal = lax.broadcasted_iota(jnp.int32, (heads, vdim), 1) == wide_row
    for s in range(seqs):
        for b in range(pieces):
            mem_out[s, b * rows : (b + 1) * rows, :] = every[s * pieces + b, 0:rows, :]
        level = every[s * pieces, rows + 8 : rows + 8 + heads, :]
        level = jnp.sum(jnp.where(diagonal, level, 0.0), axis=0, keepdims=True)
        stab_out[s : s + 1, :] = level[:, 0:heads]
        normal = jnp.concatenate([every[s * pieces + b, rows : rows + 1, 0:rows] for b in range(pieces)], axis=1)
        for h in range(heads):
            norm_out[s, h : h + 1, :] = normal[:, h * kdim : (h + 1) * kdim]
        picked = asked[s : s + 1] * select
        numer = jnp.dot(picked, mem_out[s], precision=HIGH, preferred_element_type=jnp.float32)
        inner = jnp.sum(picked * normal, axis=1, keepdims=True)
        read = numer / jnp.maximum(jnp.abs(inner), 1.0)
        for h in range(heads):
            read_out[s : s + 1, h * vdim : (h + 1) * vdim] = read[h : h + 1]

    for one in keep:
        one.wait()
    for k in range(1, size):
        gate_copy((me + k) % size).wait_send()
        key_copy((me + k) % size).wait_send()
        val_copy((me + k) % size).wait_send()
    for j in range(1, pieces):
        other = (piece + j) % pieces
        copy(part.at[other], part_got.at[piece], ps.at[other], pr.at[piece], seq * pieces + other).wait_send()
    for k in range(1, seqs):
        across(k).wait_send()
    for k in range(seqs):
        for j in range(1, pieces):
            along(k, j).wait_send()


def write_out(k_in, v_in, m_in, n_in, s_in, r_in, k_out, v_out, m_out, n_out, s_out, r_out, kb, vb, mb, reads, writes):
    chain = ((v_in, vb, v_out), (m_in, mb, m_out), (k_in, kb, k_out))
    ins = [pltpu.make_async_copy(a, b, reads.at[i]) for i, (a, b, c) in enumerate(chain)]
    outs = [pltpu.make_async_copy(b, c, writes.at[i]) for i, (a, b, c) in enumerate(chain)]
    for one in ins:
        one.start()
    n_out[...] = n_in[...]
    s_out[...] = s_in[...]
    r_out[...] = r_in[...]
    for first, then in zip(ins, outs):
        first.wait()
        then.start()
    for one in outs:
        one.wait()


def local(tokens, key_weight, value_weight, input_weight, forget_weight, forget_bias, query):
    seqs, span, width = tokens.shape
    heads = input_weight.shape[1]
    kdim = key_weight.shape[1] // heads
    vdim = value_weight.shape[1] // heads
    size = lax.axis_size("sp")
    pieces = size // seqs
    sub = span // pieces
    rows = heads * kdim // pieces
    fits = heads == 4 and pieces > 1 and heads % pieces == 0 and sub % 16 == 0 and seqs % 2 == 0
    if not fits or rows % 128 or rows > vdim or vdim % 128:
        return plain(tokens, key_weight, value_weight, input_weight, forget_weight, forget_bias, query)
    gates = jnp.concatenate([input_weight.T, forget_weight.T], axis=0)
    gates = jnp.pad(gates, ((0, 8 * heads - 2 * heads), (0, 0)))
    f32, bf16 = jnp.float32, jnp.bfloat16
    vmem = pl.BlockSpec(memory_space=pltpu.VMEM)
    hbm = pl.BlockSpec(memory_space=pltpu.HBM)
    dma = pltpu.SemaphoreType.DMA
    outs = pl.pallas_call(
        functools.partial(kernel, (seqs, span, heads, kdim, vdim, size)),
        out_shape=(
            jax.ShapeDtypeStruct((size, sub, heads * kdim), bf16),
            jax.ShapeDtypeStruct((size, sub, heads * vdim), bf16),
            jax.ShapeDtypeStruct((seqs, heads * kdim, vdim), f32),
            jax.ShapeDtypeStruct((seqs, heads, kdim), f32),
            jax.ShapeDtypeStruct((seqs, heads), f32),
            jax.ShapeDtypeStruct((seqs, heads * vdim), f32),
        ),
        in_specs=[hbm] * 3 + [vmem] * 3,
        out_specs=(hbm,) * 2 + (vmem,) * 4,
        scratch_shapes=[
            pltpu.VMEM((size, sub, heads * kdim), bf16),
            pltpu.VMEM((size, sub, heads * vdim), bf16),
            pltpu.VMEM((seqs * span, width), bf16),
            pltpu.VMEM(key_weight.shape, bf16),
            pltpu.VMEM(value_weight.shape, bf16),
            pltpu.VMEM((size, sub, heads * kdim), bf16),
            pltpu.VMEM((size, sub, heads * vdim), bf16),
            pltpu.VMEM((seqs, 2 * heads, span), f32),
            pltpu.VMEM((size, 2 * heads, span), f32),
            pltpu.VMEM((size, sub, heads * kdim), f32),
            pltpu.VMEM((heads * kdim, heads * vdim), f32),
            pltpu.VMEM((pieces, rows + 16, vdim), f32),
            pltpu.VMEM((pieces, rows + 16, vdim), f32),
            pltpu.VMEM((size, rows + 16, vdim), f32),
            dma((2,)), dma((seqs,)), dma((2,)),
            dma((size,)), dma((size,)), dma((size,)), dma((size,)), dma((size,)), dma((size,)),
            dma((pieces,)), dma((pieces,)), dma((seqs,)), dma((seqs, pieces)), dma((size,)),
        ],
        compiler_params=pltpu.CompilerParams(
            collective_id=0, has_side_effects=True, vmem_limit_bytes=63 * 1024 * 1024
        ),
    )(tokens.reshape(seqs * span, width), key_weight, value_weight, gates, forget_bias[None, :], query)
    outs = pl.pallas_call(
        write_out,
        out_shape=tuple(jax.ShapeDtypeStruct(x.shape, x.dtype) for x in outs),
        in_specs=[hbm] * 3 + [vmem] * 3,
        out_specs=(hbm,) * 3 + (vmem,) * 3,
        scratch_shapes=[pltpu.VMEM(x.shape, x.dtype) for x in (outs[0], outs[1], outs[2])]
        + [dma((3,)), dma((3,))],
        compiler_params=pltpu.CompilerParams(vmem_limit_bytes=63 * 1024 * 1024),
    )(*outs)
    keys, values, memory, normalizer, stabilizer, first_read = outs
    return (
        keys.reshape(1, size * sub, heads * kdim),
        values.reshape(1, size * sub, heads * vdim),
        memory.reshape(seqs, heads, kdim, vdim),
        normalizer,
        stabilizer,
        first_read,
    )


def solution(mesh):
    return jax.shard_map(
        local,
        mesh=mesh,
        in_specs=(
            P("gr", "sp", None),
            P(None, "tp"),
            P(None, "tp"),
            P(None, "tp"),
            P(None, "tp"),
            P("tp"),
            P("gr", "tp"),
        ),
        out_specs=(
            P(("gr", "sp"), None, "tp"),
            P(("gr", "sp"), None, "tp"),
            P("gr", "tp", None, None),
            P("gr", "tp", None),
            P("gr", "tp"),
            P("gr", "tp"),
        ),
        check_vma=False,
    )
```
